256 devices in a mesh: ep: 64 (over z, x, core), tp: 4 (over y).
Axes of the slice: x: 4, y: 4, z: 8, core: 2. Of those that a mesh axis runs over, the one named last changes fastest.
Arguments:
- queries: bfloat16 [16384, 2, 1024], P('ep', None, 'tp')
- keys: bfloat16 [16384, 2, 256], P('ep', None, 'tp')
- values: bfloat16 [16384, 2, 256], P('ep', None, 'tp'), may hold values from -6 to 6
- query_gain: float32 [64], replicated, may hold values from 1.2 to 6
- key_gain: float32 [64], replicated, may hold values from 1.2 to 6
- out_weight: bfloat16 [1024, 2048], P('tp'), may hold values from -0.75 to 0.75
- moe_tokens: bfloat16 [32768, 2048], P(('ep', 'tp')), may hold values from -6 to 6
- moe_gain: float32 [2048], replicated, may hold values from 0.1 to 1.9
- routes: int32 [32768, 2], P(('ep', 'tp')), may hold values from 0 to 63, all different within a row; in each aligned block of 128 rows (0 to 127, 128 to 255, ...) at most 6 rows name the same one
- route_weight: float32 [32768, 2], P(('ep', 'tp')), may hold values from 0.1 to 1
- w_gate: bfloat16 [64, 2048, 1024], P('ep', None, 'tp'), may hold values from -0.125 to 0.125
- w_up: bfloat16 [64, 2048, 1024], P('ep', None, 'tp'), may hold values from -0.125 to 0.125
- w_down: bfloat16 [64, 1024, 2048], P('ep', 'tp'), may hold values from -0.1875 to 0.1875
Outputs:
- attended: bfloat16 [16384, 2, 2048], P(('ep', 'tp'))
- routed: bfloat16 [32768, 2048], P(('ep', 'tp'))
The draws below stay inside these ranges and needn't reach their ends.
Inputs may be any that keep to these rules, and one draw needn't show every extreme that they name: `routes`: each row names 2 different experts. The rows of one device name no expert more than 6 times, and in every draw some device's rows name one expert exactly 6 times.
All inputs are finite; a program needn't handle non-finite values.
Results may differ from the reference program's by a relative error of at most 0.013.
The reference program's roundings to bfloat16 on the way count: a program that leaves them out, or rounds other values in their place, can miss the bound.
Values may be sent and summed in bfloat16 or wider, within the bound.
No kernel may reach another device: no remote copies, remote signals or barrier semaphores. Data moves between devices by JAX's collectives and lax.ppermute only.
A program may use at most 128 MiB of HBM per device.

```python
import math
import jax
import jax.numpy as jnp
import numpy as np
from jax import lax

D = 2048
HEADS = 16
KV_HEADS = 4
HEAD_DIM = 64
FF = 1024
TOPK = 2
GRID_W = 64
SEQS = 2
TOK_DEV = 128
LEN = 16384
EXPERTS = 64
CAP = 6
TOKENS = 32768
N_EP = 64
N_TP = 4


def draw_both(key):
    keys_drawn = jax.random.normal(jax.random.fold_in(key, 12), (LEN, SEQS, KV_HEADS * HEAD_DIM), jnp.float32)
    queries_drawn = jax.random.normal(jax.random.fold_in(key, 11), (LEN, SEQS, HEADS * HEAD_DIM), jnp.float32)
    return (queries_drawn, keys_drawn)


def draw_queries(key, part):
    return draw_both(key)[0].astype(jnp.bfloat16)


def draw_keys(key, part):
    return draw_both(key)[1].astype(jnp.bfloat16)


def draw_gain_values(key):
    return jax.random.uniform(key, (HEAD_DIM,), jnp.float32, 1.2, 2.0)


def draw_query_gain(key, part):
    return draw_gain_values(jax.random.fold_in(key, 21))


def draw_key_gain(key, part):
    return draw_gain_values(jax.random.fold_in(key, 22))


def shard_levels(own_key, shape, split, least, high):
    def one(position, blocks):
        draws = jax.random.uniform(jax.random.fold_in(jax.random.fold_in(own_key, 6), position), (blocks,), jnp.float32, least / len(split), high / len(split))
        return jnp.repeat(jnp.exp(draws), shape[position] // blocks).reshape((-1,) + (1,) * (len(shape) - position - 1))

    level = one(*split[0])
    for cut in split[1:]:
        level = level * one(*cut)
    return level


def shared_out(key, own, number, rows, count, top, limit, skew):
    order = jax.random.permutation(key, count)
    heavy_load, common = load_shares(count, rows * top, limit, skew, True), load_shares(count, rows * top, limit, skew, False)
    places = jnp.arange(count)

    def named(sizes, turn):
        used = int((sizes > 0).sum())
        fixed = max(1, used // 4)
        passed = fixed + (places - fixed + turn * (used - fixed)) % max(1, count - fixed)
        return jnp.zeros((count,), jnp.int32).at[order[jnp.where(places < fixed, places, passed)]].set(jnp.asarray(sizes, jnp.int32))

    sizes = jnp.where(number % 4 == 0, named(heavy_load, number // 4), named(common, number - number // 4 - 1))
    mixed = jax.random.permutation(jax.random.fold_in(own, 3), count)
    source_of, sink = mixed[0:count // 2 * 2:2], mixed[1:count // 2 * 2:2]
    margin = jnp.minimum(sizes[source_of] - 1, limit - sizes[sink]) // 2
    margin = jnp.where((source_of == order[0]) | (sink == order[0]) | (sizes[sink] == 0), 0, jnp.maximum(margin, 0))
    passed = jax.random.randint(jax.random.fold_in(own, 4), (count // 2,), 0, 1 << 20) % (margin + 1)
    sizes = sizes.at[source_of].add(-passed).at[sink].add(passed)
    members = jnp.searchsorted(jnp.cumsum(sizes), jnp.arange(rows * top), side="right").astype(jnp.int32)
    table = members.reshape(top, rows).T
    table = table[jax.random.permutation(jax.random.fold_in(own, 1), rows)]
    turn = jax.random.randint(jax.random.fold_in(own, 2), (rows, 1), 0, top)
    return jnp.take_along_axis(table, (jnp.arange(top)[None, :] + turn) % top, axis=1)


def load_shares(number_of, total, most, slope, full):
    weights = [(1 << 20) // math.isqrt(standing ** slope) + 1 for standing in range(1, number_of + 1)]
    largest = most if full else min(most, max(-(-total // number_of), total * weights[0] // sum(weights)))
    least = 1 if total - largest >= number_of - 1 else 0
    counts, spare = [largest] + [least] * (number_of - 1), total - largest - least * (number_of - 1)
    while spare > 0:
        movable = [i for i in range(1, number_of) if counts[i] < largest] or [i for i in range(1, number_of) if counts[i] < most]
        whole, budget = sum([weights[i] for i in movable]), spare
        for i in movable:
            addition = min(most - counts[i], max(1, budget * weights[i] // whole), spare)
            counts[i] = counts[i] + addition
            spare = spare - addition
    return np.array(counts)


def normal_values(rng, shape, scale, limit, cuts=(), held_as=jnp.bfloat16):
    result = scale * jax.random.normal(rng, shape, jnp.float32)
    if cuts:
        result = result * shard_levels(rng, shape, cuts, -0.22, 0.18)
    return jnp.clip(result, -limit, limit).astype(held_as)


def setup_inputs(seed: int = 0) -> dict:
    seeds = jax.random.split(jax.random.key(seed), 14)
    queries = draw_queries(jax.random.fold_in(seeds[13], 71), 0)
    keys = draw_keys(jax.random.fold_in(seeds[13], 71), 0)
    values = normal_values(seeds[2], (LEN, SEQS, KV_HEADS * HEAD_DIM), 1.0, 6.0, ((0, 64), (2, 4)))
    query_gain = draw_query_gain(jax.random.fold_in(seeds[13], 71), 0)
    key_gain = draw_key_gain(jax.random.fold_in(seeds[13], 71), 0)
    out_weight = normal_values(seeds[5], (HEADS * HEAD_DIM, D), (HEADS * HEAD_DIM // 16) ** -0.5, 0.75, ((0, 4),))
    moe_tokens = normal_values(seeds[6], (TOKENS, D), 1.0, 6.0, ((0, 256),))
    moe_gain = jnp.clip(1.0 + 0.18 * jax.random.normal(seeds[7], (D,), jnp.float32), 0.1, 1.9)
    routes_keys = jax.random.split(jax.random.fold_in(seeds[8], 1), TOKENS // TOK_DEV)
    routes_turns = jax.random.permutation(jax.random.fold_in(seeds[8], 3), TOKENS // TOK_DEV)
    routes = jax.vmap(lambda own, number: shared_out(jax.random.fold_in(seeds[8], 2), own, number, TOK_DEV, EXPERTS, TOPK, CAP, 1))(routes_keys, routes_turns).reshape((TOKENS, TOPK))
    route_weight = jnp.clip(0.1 + 0.9 * jax.random.uniform(seeds[9], (TOKENS, TOPK), jnp.float32) ** shard_levels(seeds[9], (TOKENS, TOPK), ((0, 256),), -0.2, 0.2), 0.1, 1.0)
    w_gate = normal_values(seeds[10], (EXPERTS, D, FF), D ** -0.5, 0.125, ((0, 64), (2, 4)))
    w_up = normal_values(seeds[11], (EXPERTS, D, FF), D ** -0.5, 0.125, ((0, 64), (2, 4)))
    w_down = normal_values(seeds[12], (EXPERTS, FF, D), FF ** -0.5, 0.1875, ((0, 64), (1, 4)))
    return dict(queries=queries, keys=keys, values=values, query_gain=query_gain, key_gain=key_gain, out_weight=out_weight, moe_tokens=moe_tokens, moe_gain=moe_gain, routes=routes, route_weight=route_weight, w_gate=w_gate, w_up=w_up, w_down=w_down)


EPS = 1e-06
THETA = 10000.0

def turn(normed, positions):
    quarter = normed.shape[-1] // 4
    inverse = THETA ** (-jnp.arange(quarter, dtype=jnp.float32) / quarter)
    grid_row = (positions // GRID_W).astype(jnp.float32)
    grid_col = (positions % GRID_W).astype(jnp.float32)
    angles = jnp.stack([grid_row[:, None] * inverse, grid_col[:, None] * inverse], axis=1)
    cosine = jnp.cos(angles)[:, None, None]
    sine = jnp.sin(angles)[:, None, None]
    parts = normed.reshape(normed.shape[:-1] + (2, 2, quarter))
    first = parts[..., 0, :]
    second = parts[..., 1, :]
    turned = jnp.stack([first * cosine - second * sine, second * cosine + first * sine], axis=-2)
    return turned.reshape(normed.shape)

def prepare(data, positions, gain):
    heads = data.astype(jnp.float32).reshape(data.shape[0], data.shape[1], -1, HEAD_DIM)
    normed = heads * lax.rsqrt(lax.optimization_barrier(jnp.mean(heads * heads, axis=-1, keepdims=True)) + EPS) * gain
    return turn(normed, positions).astype(jnp.bfloat16)

def reference(queries, keys, values, query_gain, key_gain, out_weight, moe_tokens, moe_gain, routes, route_weight, w_gate, w_up, w_down):
    positions = jnp.arange(LEN, dtype=jnp.int32)
    q_rot = prepare(queries, positions, query_gain)
    k_rot = prepare(keys, positions, key_gain)
    key_float = k_rot.astype(jnp.float32)
    value_float = values.reshape(LEN, SEQS, KV_HEADS, HEAD_DIM).astype(jnp.float32)
    groups = HEADS // KV_HEADS
    block = math.gcd(LEN, 64)
    query_blocks = q_rot.reshape(LEN // block, block, SEQS, KV_HEADS, groups, HEAD_DIM)

    def attend(query_block):
        scores = jnp.einsum('bskgd,lskd->skgbl', query_block.astype(jnp.float32), key_float) * HEAD_DIM ** (-0.5)
        largest = lax.optimization_barrier(jnp.max(scores, axis=-1, keepdims=True))
        expo = jnp.exp(scores - largest)
        total = lax.optimization_barrier(jnp.sum(expo, axis=-1))
        probs = lax.optimization_barrier(expo.astype(jnp.bfloat16)).astype(jnp.float32)
        summed = jnp.einsum('skgbl,lskd->skgbd', probs, value_float) / total[..., None]
        return jnp.transpose(summed, (3, 0, 1, 2, 4)).astype(jnp.bfloat16)
    mixed = lax.map(attend, query_blocks).reshape(LEN * SEQS, HEADS * HEAD_DIM)
    width = HEADS * HEAD_DIM // N_TP
    accum = jnp.zeros((LEN * SEQS, D), jnp.float32)
    for index in range(N_TP):
        part = jnp.dot(mixed[:, index * width:(index + 1) * width], out_weight[index * width:(index + 1) * width], preferred_element_type=jnp.float32)
        accum = accum + lax.optimization_barrier(part.astype(jnp.bfloat16)).astype(jnp.float32)
    attended = accum.astype(jnp.bfloat16).reshape(LEN, SEQS, D)
    token_float = moe_tokens.astype(jnp.float32)
    normed = (token_float * lax.rsqrt(lax.optimization_barrier(jnp.mean(token_float * token_float, axis=-1, keepdims=True)) + EPS) * moe_gain).astype(jnp.bfloat16)
    most = N_EP * N_TP * CAP
    unit_width = FF // N_TP

    def expert(carry, item):
        index, gate_weight, up_weight, down_weight = item
        chosen = routes == index
        weight = lax.optimization_barrier(jnp.sum(jnp.where(chosen, route_weight, 0.0), axis=1))
        live = jnp.any(chosen, axis=1)
        rows = jnp.nonzero(live, size=most, fill_value=0)[0].astype(jnp.int32)
        count = jnp.sum(live.astype(jnp.int32))
        valid = (jnp.arange(most, dtype=jnp.int32) < count).astype(jnp.float32)
        picked = normed[rows]
        gate = jnp.dot(picked, gate_weight, preferred_element_type=jnp.float32)
        up = jnp.dot(picked, up_weight, preferred_element_type=jnp.float32)
        hidden = (jax.nn.silu(gate) * up).astype(jnp.bfloat16)
        out = jnp.zeros((most, D), jnp.float32)
        for block_index in range(N_TP):
            part = jnp.dot(hidden[:, block_index * unit_width:(block_index + 1) * unit_width], down_weight[block_index * unit_width:(block_index + 1) * unit_width], preferred_element_type=jnp.float32)
            out = out + lax.optimization_barrier(part.astype(jnp.bfloat16)).astype(jnp.float32)
        expert_out = lax.optimization_barrier(out.astype(jnp.bfloat16)).astype(jnp.float32)
        contrib = expert_out * (weight[rows] * valid)[:, None]
        return (carry.at[rows].add(contrib), None)
    routed, _ = lax.scan(expert, jnp.zeros((TOKENS, D), jnp.float32), (jnp.arange(EXPERTS, dtype=jnp.int32), w_gate, w_up, w_down))
    return (attended, routed.astype(jnp.bfloat16))
```

```python
import functools

import jax
import jax.numpy as jnp
from jax import lax
from jax.experimental import pallas as pl
from jax.experimental.pallas import tpu as pltpu
from jax.sharding import Mesh, PartitionSpec as P


HEAD_DIM = 64
GRID_W = 64
EPS = 1e-06
THETA = 10000.0
LOG2E = 1.4426950408889634
PARTS = 2


def attend_kernel(*refs, first, last, per, chunk, width, lead, lag):
    q_ref, kv_ref = refs[:2]
    given = () if first else refs[2:4]
    outs = refs[2 if first else 4 :]
    if last:
        o_ref, kd, m_ref, acc_ref, s_ref, x_ref = outs
    else:
        m_ref, acc_ref, kd, s_ref, x_ref = outs
    blocks, _, length = kv_ref.shape
    total = q_ref.shape[1]

    def flip(i, c):
        keys = jnp.transpose(kv_ref[i, :HEAD_DIM, :].astype(jnp.float32)).astype(jnp.bfloat16)
        kd[pl.ds(pl.multiple_of(i * length, length), length), :] = jnp.concatenate([keys, keys], axis=1)
        return c

    lax.fori_loop(0, blocks, flip, 0)
    if first:
        m_ref[...] = jnp.full_like(m_ref, -1e30)
        acc_ref[...] = jnp.zeros_like(acc_ref)
    else:
        m_ref[...] = given[0][...]
        acc_ref[...] = given[1][...]
    units = [
        (b, s, n) for b in range(per) for s in range(length // chunk) for n in range(total // width)
    ]
    count = len(units)
    slots = s_ref.shape[0]
    final = blocks * length - chunk

    def scores(i, u):
        slot = u % slots
        wrap, u = divmod(u, count)
        b, s, n = units[u]
        at = ((i + wrap) * per + b) * length + s * chunk
        if wrap:
            at = jnp.minimum(at, final)
        made = jnp.dot(
            kd[pl.ds(pl.multiple_of(at, chunk), chunk), :],
            q_ref[:, n * width : (n + 1) * width],
            preferred_element_type=jnp.float32,
        )
        s_ref[slot] = made
        x_ref[slot] = jnp.max(made, axis=0, keepdims=True)

    def soften(u):
        n = units[u][2]
        cols = slice(n * width, (n + 1) * width)
        before = m_ref[:, cols]
        best = jnp.maximum(before, x_ref[u % slots])
        m_ref[:, cols] = best
        return jnp.exp2(s_ref[u % slots] - best).astype(jnp.bfloat16), jnp.exp2(before - best)

    def mix(i, u, probs, factor):
        b, s, n = units[u]
        cols = slice(n * width, (n + 1) * width)
        vals = kv_ref[i * per + b, HEAD_DIM:, s * chunk : (s + 1) * chunk]
        vals = jnp.concatenate([vals, jnp.ones((16, chunk), jnp.bfloat16)], axis=0)
        added = jnp.dot(vals, probs, preferred_element_type=jnp.float32)
        acc_ref[:, cols] = acc_ref[:, cols] * factor + added

    for u in range(lead):
        scores(0, u)

    def body(i, c):
        pending = []
        for u in range(count):
            scores(i, u + lead)
            pending.append((u, *soften(u)))
            if len(pending) > lag:
                mix(i, *pending.pop(0))
        for item in pending:
            mix(i, *item)
        return c

    lax.fori_loop(0, blocks // per, body, 0)
    if last:
        o_ref[...] = (acc_ref[:HEAD_DIM, :] / acc_ref[HEAD_DIM : HEAD_DIM + 1, :]).astype(o_ref.dtype)


def attend(q, kv, part, parts, state):
    whole, features, length = kv.shape
    blocks = whole // parts
    total = q.shape[1]
    chunk, width, slots = length, 256, 8
    first, last = part == 0, part == parts - 1
    sums = (1, total), (HEAD_DIM + 16, total)
    in_specs = [
        pl.BlockSpec((2 * HEAD_DIM, total), lambda i: (0, 0)),
        pl.BlockSpec((blocks, features, length), lambda i: (part, 0, 0)),
    ] + [pl.BlockSpec(s, lambda i: (0, 0)) for s in sums if not first]
    if last:
        out_shape = jax.ShapeDtypeStruct((HEAD_DIM, total), jnp.bfloat16)
        out_specs = pl.BlockSpec((HEAD_DIM, total), lambda i: (0, 0))
    else:
        out_shape = tuple(jax.ShapeDtypeStruct(s, jnp.float32) for s in sums)
        out_specs = tuple(pl.BlockSpec(s, lambda i: (0, 0)) for s in sums)
    kd = pltpu.VMEM((blocks * length, 2 * HEAD_DIM), jnp.bfloat16)
    work = [pltpu.VMEM((slots, chunk, width), jnp.float32), pltpu.VMEM((slots, 1, width), jnp.float32)]
    held = [pltpu.VMEM(s, jnp.float32) for s in sums]
    return pl.pallas_call(
        functools.partial(
            attend_kernel, first=first, last=last, per=1, chunk=chunk, width=width, lead=3, lag=1
        ),
        grid=(1,),
        out_shape=out_shape,
        in_specs=in_specs,
        out_specs=out_specs,
        scratch_shapes=[kd, *held, *work] if last else [kd, *work],
        compiler_params=pltpu.CompilerParams(vmem_limit_bytes=32 * 2**20),
        cost_estimate=pl.CostEstimate(
            flops=16 * total * blocks * length * HEAD_DIM,
            bytes_accessed=8 * 2**20 // parts,
            transcendentals=total * blocks * length,
        ),
        name="attend",
    )(q, kv, *state)


def route_kernel(x_ref, gain_ref, routes_ref, o_ref, slot_ref, *, experts, deep):
    tokens, width = x_ref.shape
    top = routes_ref.shape[0]
    data = x_ref[...].astype(jnp.float32)
    normed = data * lax.rsqrt(jnp.mean(data * data, axis=-1, keepdims=True) + EPS) * gain_ref[...]
    normed = normed.astype(jnp.bfloat16)
    expert_id = lax.broadcasted_iota(jnp.int32, (experts, tokens), 0)
    one = lax.broadcasted_iota(jnp.int32, (tokens, tokens), 0)
    two = lax.broadcasted_iota(jnp.int32, (tokens, tokens), 1)
    earlier = jnp.where(one < two, 1.0, 0.0).astype(jnp.bfloat16)
    held = jnp.zeros((experts, 1), jnp.float32)
    slots = []
    for k in range(top):
        chosen = routes_ref[k : k + 1, :]
        hits = jnp.where(expert_id == chosen, 1.0, 0.0)
        before = held + jnp.dot(hits.astype(jnp.bfloat16), earlier, preferred_element_type=jnp.float32)
        rank = jnp.sum(hits * before, axis=0, keepdims=True).astype(jnp.int32)
        held = held + jnp.sum(hits, axis=1, keepdims=True)
        slots.append((rank // 2) * (2 * experts) + chosen * 2 + rank % 2)
        slot_ref[k : k + 1, :] = slots[k]
    row = lax.broadcasted_iota(jnp.int32, (2 * experts, tokens), 0)
    for d in range(deep):
        pick = jnp.zeros((2 * experts, tokens), jnp.float32)
        for slot in slots:
            pick = pick + jnp.where(row + d * 2 * experts == slot, 1.0, 0.0)
        rows = jnp.dot(pick.astype(jnp.bfloat16), normed, preferred_element_type=jnp.float32)
        o_ref[:, d * width : (d + 1) * width] = rows.astype(o_ref.dtype)


def route(tokens, gain, routes, experts, deep):
    count, width = tokens.shape
    return pl.pallas_call(
        functools.partial(route_kernel, experts=experts, deep=deep),
        out_shape=(
            jax.ShapeDtypeStruct((2 * experts, deep * width), jnp.bfloat16),
            jax.ShapeDtypeStruct(routes.shape, jnp.int32),
        ),
        compiler_params=pltpu.CompilerParams(vmem_limit_bytes=16 * 2**20),
        cost_estimate=pl.CostEstimate(
            flops=4 * experts * deep * count * width, bytes_accessed=2 * 2**20, transcendentals=0
        ),
        name="route",
    )(tokens, gain, routes)


def combine_kernel(rows_ref, slot_ref, weight_ref, o_ref, *, deep):
    count, wide = rows_ref.shape
    width = wide // deep
    tokens, top = slot_ref.shape
    row = lax.broadcasted_iota(jnp.int32, (tokens, count), 1)
    summed = jnp.zeros((tokens, width), jnp.float32)
    for k in range(top):
        picked = jnp.zeros((tokens, width), jnp.float32)
        for d in range(deep):
            pick = jnp.where(row + d * count == slot_ref[:, k : k + 1], 1.0, 0.0).astype(jnp.bfloat16)
            picked = picked + jnp.dot(
                pick, rows_ref[:, d * width : (d + 1) * width], preferred_element_type=jnp.float32
            )
        summed = summed + picked * weight_ref[:, k : k + 1]
    o_ref[...] = summed.astype(o_ref.dtype)


def combine(rows, slots, weights, deep):
    tokens = slots.shape[0]
    count, wide = rows.shape
    return pl.pallas_call(
        functools.partial(combine_kernel, deep=deep),
        out_shape=jax.ShapeDtypeStruct((tokens, wide // deep), jnp.bfloat16),
        compiler_params=pltpu.CompilerParams(vmem_limit_bytes=16 * 2**20),
        cost_estimate=pl.CostEstimate(
            flops=4 * tokens * count * wide, bytes_accessed=2 * 2**20, transcendentals=0
        ),
        name="combine",
    )(rows, slots, weights)


def expert_kernel(x_ref, *refs, deep, shards, pieces, carried):
    take = lambda group: jnp.concatenate([r[...] for r in group], axis=0)
    weights = refs[: 3 * shards * pieces]
    rest = refs[3 * shards * pieces :]
    o_ref = rest[-1]
    count = x_ref.shape[0]
    width = x_ref.shape[1] // deep
    rows = jnp.concatenate([x_ref[:, d * width : (d + 1) * width] for d in range(deep)], axis=0)
    total = None
    for i in range(shards):
        gate_w, up_w, down_w = (
            take(weights[(3 * i + j) * pieces : (3 * i + j + 1) * pieces]) for j in range(3)
        )
        gate = jnp.dot(rows, gate_w, preferred_element_type=jnp.float32)
        up = jnp.dot(rows, up_w, preferred_element_type=jnp.float32)
        hidden = (gate * jax.nn.sigmoid(gate) * up).astype(jnp.bfloat16)
        part = jnp.dot(hidden, down_w, preferred_element_type=jnp.float32)
        part = part.astype(jnp.bfloat16).astype(jnp.float32)
        total = part if total is None else total + part
    if carried:
        total = total + rest[0][...]
        for d in range(deep):
            o_ref[:, d * width : (d + 1) * width] = total[d * count : (d + 1) * count].astype(o_ref.dtype)
    else:
        o_ref[...] = total


def expert(rows, weights, deep, pieces, carried=()):
    count, wide = rows.shape
    flat = [piece for shard in weights for kind in shard for piece in kind]
    units = flat[0].shape[1]
    shards = len(weights)
    if carried:
        out_shape = jax.ShapeDtypeStruct((count, wide), jnp.bfloat16)
    else:
        out_shape = jax.ShapeDtypeStruct((count * deep, wide // deep), jnp.float32)
    return pl.pallas_call(
        functools.partial(
            expert_kernel, deep=deep, shards=shards, pieces=pieces, carried=len(carried)
        ),
        out_shape=out_shape,
        compiler_params=pltpu.CompilerParams(vmem_limit_bytes=32 * 2**20),
        cost_estimate=pl.CostEstimate(
            flops=6 * count * wide * units * shards,
            bytes_accessed=6 * (wide // deep) * units * shards,
            transcendentals=0,
        ),
        name="expert",
    )(rows, *flat, *carried)


def turned(data, gain, cosine, sine):
    normed = data * lax.rsqrt(jnp.mean(data * data, axis=1, keepdims=True) + EPS) * gain[:, None]
    parts = normed.reshape(data.shape[0], 2, 2, HEAD_DIM // 4, data.shape[2])
    first, second = parts[:, :, 0], parts[:, :, 1]
    out = jnp.stack([first * cosine - second * sine, second * cosine + first * sine], axis=2)
    return out.reshape(data.shape)


def layer(
    queries,
    keys,
    values,
    query_gain,
    key_gain,
    out_weight,
    moe_tokens,
    moe_gain,
    routes,
    route_weight,
    w_gate,
    w_up,
    w_down,
):
    ep = ("z", "x", "c")
    tp = lax.axis_size("y")
    experts = lax.axis_size(ep)
    swap_c = [(0, 1), (1, 0)]
    right = [(i, (i + 1) % tp) for i in range(tp)]
    left = [(i, (i - 1) % tp) for i in range(tp)]
    core = lax.axis_index("c")

    own, from_left, from_right, opposite = [], [], [], []
    for weight in (w_gate[0], w_up[0], w_down[0]):
        came_left = lax.ppermute(weight, "y", right)
        came_right = lax.ppermute(weight, "y", left)
        middle = weight.shape[0] // 2
        upper = lax.ppermute(came_left[:middle], "y", right)
        lower = lax.ppermute(came_right[middle:], "y", left)
        own.append((weight,))
        from_left.append((came_left,))
        from_right.append((came_right,))
        opposite.append((upper, lower))

    tok_count, width = moe_tokens.shape
    top = routes.shape[1]
    capacity = max(2, (3 * tok_count * top + 2 * experts - 1) // (2 * experts))
    deep = -(-capacity // 2)
    rows, slots = route(moe_tokens, moe_gain[None], routes.T, experts, deep)
    sent = lax.all_to_all(
        rows.reshape(experts, 2, deep * width), ep, split_axis=0, concat_axis=0, tiled=True
    )

    pos_count = queries.shape[0]
    chip = lax.axis_index("z") * lax.axis_size("x") + lax.axis_index("x")
    k_t = jnp.transpose(keys, (1, 2, 0))
    v_t = jnp.transpose(values, (1, 2, 0))
    kv = jnp.concatenate([k_t, v_t], axis=1)
    q_t = jnp.transpose(queries, (1, 2, 0))
    mine = lambda a: lax.dynamic_index_in_dim(a, core, 0, keepdims=False)
    other = lambda a: lax.dynamic_index_in_dim(a, 1 - core, 0, keepdims=False)
    kv_got = lax.ppermute(other(kv), "c", swap_c)
    q_got = lax.ppermute(other(q_t), "c", swap_c)

    def in_order(own, got):
        low = jnp.where(core == 0, own, got)
        high = jnp.where(core == 0, got, own)
        return jnp.concatenate([low, high], axis=-1)

    kv_chip = in_order(mine(kv), kv_got)
    q_chip = in_order(mine(q_t), q_got)
    span = 2 * pos_count
    quarter = HEAD_DIM // 4
    inverse = THETA ** (-jnp.arange(quarter, dtype=jnp.float32) / quarter)
    positions = chip * span + jnp.arange(span, dtype=jnp.int32)
    grid = jnp.stack([positions // GRID_W, positions % GRID_W]).astype(jnp.float32)
    angles = grid[:, None, :] * inverse[None, :, None]
    cosine, sine = jnp.cos(angles), jnp.sin(angles)
    k_rot = turned(kv_chip[None, :HEAD_DIM].astype(jnp.float32), key_gain, cosine, sine)[0]
    kv_local = jnp.concatenate([k_rot.astype(jnp.bfloat16), kv_chip[HEAD_DIM:]], axis=0)
    kv_all = lax.all_gather(kv_local, ("z", "x"))
    heads = q_chip.shape[0] // HEAD_DIM
    q_rot = turned(
        q_chip.reshape(heads, HEAD_DIM, span).astype(jnp.float32), query_gain, cosine, sine
    ).astype(jnp.bfloat16)
    scaled = q_rot.astype(jnp.float32) * (HEAD_DIM**-0.5 * LOG2E)
    high = scaled.astype(jnp.bfloat16)
    low = (scaled - high.astype(jnp.float32)).astype(jnp.bfloat16)
    q_pair = jnp.concatenate([high, low], axis=1)
    q_pair = jnp.transpose(q_pair, (1, 0, 2)).reshape(2 * HEAD_DIM, heads * span)
    state = ()
    for part in range(PARTS):
        state = attend(q_pair, kv_all, part, PARTS, state)
    mixed = state.reshape(HEAD_DIM, heads, span)

    share = pos_count // tp
    blocks = mixed.reshape(HEAD_DIM, heads, 2, tp, share)
    blocks = jnp.transpose(blocks, (2, 3, 4, 1, 0)).reshape(2 * tp, share, heads * HEAD_DIM)
    place = core * tp + lax.axis_index("y")
    arrived = [lax.dynamic_index_in_dim(blocks, place, 0, keepdims=False)]
    for step in range(1, 2 * tp):
        block = lax.dynamic_index_in_dim(blocks, place ^ step, 0, keepdims=False)
        arrived.append(lax.ppermute(block, ("c", "y"), [(i, i ^ step) for i in range(2 * tp)]))
    arrived = jnp.stack(arrived)
    arrived = jnp.stack(
        [lax.dynamic_index_in_dim(arrived, place ^ i, 0, keepdims=False) for i in range(2 * tp)]
    )
    arrived = arrived.reshape(2, tp, share, heads * HEAD_DIM)
    whole_weight = lax.all_gather(out_weight, "y")
    summed = 0.0
    for i in range(tp):
        rows = jnp.transpose(arrived[:, i], (1, 0, 2)).reshape(share * 2, heads * HEAD_DIM)
        part = jnp.dot(rows, whole_weight[i], preferred_element_type=jnp.float32)
        summed = summed + part.astype(jnp.bfloat16).astype(jnp.float32)
    attended = summed.astype(jnp.bfloat16).reshape(share, 2, -1)

    rows = sent.reshape(2 * experts, deep * width)
    partial = expert(rows, (own, from_left, from_right), deep, 1)
    result = expert(rows, (opposite,), deep, 2, (partial,))
    returned = lax.all_to_all(
        result.reshape(experts, 2, deep * width), ep, split_axis=0, concat_axis=0, tiled=True
    )
    routed = combine(returned.reshape(2 * experts, deep * width), slots.T, route_weight, deep)
    return (attended, routed)


def solution(mesh):
    ep, tp = mesh.devices.shape
    split = Mesh(mesh.devices.reshape(8, ep // 16, 2, tp), ("z", "x", "c", "y"))
    rows = ("z", "x", "c")
    in_specs = (
        P(rows, None, "y"),
        P(rows, None, "y"),
        P(rows, None, "y"),
        P(),
        P(),
        P("y", None),
        P((*rows, "y"), None),
        P(),
        P((*rows, "y"), None),
        P((*rows, "y"), None),
        P(rows, None, "y"),
        P(rows, None, "y"),
        P(rows, "y", None),
    )
    out_specs = (P((*rows, "y"), None, None), P((*rows, "y"), None))
    return jax.shard_map(layer, mesh=split, in_specs=in_specs, out_specs=out_specs, check_vma=False)
```
